256 devices in a mesh: ep: 16 (over y, x), tp: 16 (over z, core).
Axes of the slice: x: 4, y: 4, z: 8, core: 2. Of those that a mesh axis runs over, the one named last changes fastest.
Arguments:
- queries: bfloat16 [2, 1024, 16384], P(None, 'tp', 'ep'), may hold values from -6 to 6
- key_vectors: bfloat16 [2, 1024, 16384], P(None, 'tp', 'ep'), may hold values from -6 to 6
- value_vectors: bfloat16 [2, 1024, 16384], P(None, 'tp', 'ep'), may hold values from -12 to 12
- cumulative_gate: float32 [2, 16, 16384], P(None, 'tp'), may hold values from -16384 to 0, as said below
- expert_input: bfloat16 [32768, 2048], P(('ep', 'tp')), may hold values from -6 to 6
- norm_gain: float32 [2048], replicated, may hold values from 0.1 to 1.9
- group_choice: int32 [32768], P(('ep', 'tp')), may hold values from 0 to 15, as said below
- group_weight: float32 [32768], P(('ep', 'tp')), may hold values from 0.3 to 1
- expert_logits: float32 [32768, 2], P(('ep', 'tp')), may hold values from -6 to 6
- gate_weight: bfloat16 [32, 2048, 2048], P('ep', 'tp'), may hold values from -0.125 to 0.125
- up_weight: bfloat16 [32, 2048, 2048], P('ep', 'tp'), may hold values from -0.125 to 0.125
- down_weight: bfloat16 [32, 2048, 2048], P('ep', 'tp'), may hold values from -0.25 to 0.25
Outputs:
- attention: bfloat16 [2, 1024, 16384], P(None, 'tp', 'ep')
- expert_output: bfloat16 [32768, 2048], P(('ep', 'tp'))
The draws below stay inside these ranges and needn't reach their ends.
Inputs may be any that keep to these rules, and one draw needn't show every extreme that they name: `cumulative_gate`: each row is non-increasing along positions. `group_choice`: in each aligned block of 128 rows (the rows of one device) no group is named more than 10 times, and one group is named exactly 10 times in every block.
All inputs are finite; a program needn't handle non-finite values.
Results may differ from the reference program's by a relative error of at most 0.017.
Values may be sent and summed in bfloat16 or wider, within the bound.
A program may use at most 128 MiB of HBM per device.

```python
import math
import jax
import jax.numpy as jnp
from jax import lax

D = 2048
HEADS = 16
HEAD = 64
HD = 1024
FE = 2048
EPG = 2
STRAND_TOTAL = 2
SEG = 1024
STRAND_SPAN = 16384
TOK_DEV = 128
MOE_TOKENS = 32768
GROUPS = 16
EXPERTS = 32
CAP = 10
N_TP = 16


def draw_queries(key, part):
    rows = jnp.clip(1.6 * jax.random.normal(jax.random.fold_in(key, 11), (STRAND_TOTAL, STRAND_SPAN, HD), jnp.float32), -6.0, 6.0)
    return jnp.transpose(rows, (0, 2, 1)).astype(jnp.bfloat16)


def draw_key_vectors(key, part):
    rows = jnp.clip(1.6 * jax.random.normal(jax.random.fold_in(key, 12), (STRAND_TOTAL, STRAND_SPAN, HD), jnp.float32), -6.0, 6.0)
    return jnp.transpose(rows, (0, 2, 1)).astype(jnp.bfloat16)


def draw_cumulative_gate(key, part):
    order = jax.random.permutation(jax.random.fold_in(key, 21), HEADS).astype(jnp.int32)
    fast_span = jnp.exp(jax.random.uniform(jax.random.fold_in(key, 23), (STRAND_TOTAL, HEADS), jnp.float32, math.log(30.0), math.log(100.0)))
    slow = order[None, :] < HEADS // 2
    slow_total = jnp.exp(jax.random.uniform(jax.random.fold_in(key, 22), (STRAND_TOTAL, HEADS), jnp.float32, math.log(0.25), math.log(0.8)))
    rate = jnp.where(slow, slow_total / STRAND_SPAN, 1.0 / fast_span)
    block_factor = jnp.exp(jax.random.uniform(jax.random.fold_in(key, 24), (STRAND_TOTAL, 1, STRAND_SPAN // SEG), jnp.float32, math.log(0.5), math.log(2.0)))
    block_factor = jnp.repeat(block_factor, SEG, axis=2)
    jitter = jax.random.uniform(jax.random.fold_in(key, 25), (STRAND_TOTAL, HEADS, STRAND_SPAN), jnp.float32, 0.1, 1.9)
    pass_tally = -rate[:, :, None] * block_factor * jitter
    stretch_shift = jax.random.randint(jax.random.fold_in(key, 26), (STRAND_TOTAL, 2), 1, STRAND_SPAN).astype(jnp.int32)
    stretch_width = jax.random.uniform(jax.random.fold_in(key, 27), (STRAND_TOTAL, 2), jnp.float32, 0.22, 0.69)
    strand_number = jnp.arange(STRAND_TOTAL, dtype=jnp.int32)[:, None]
    stretch_table = jnp.zeros((STRAND_TOTAL, STRAND_SPAN), jnp.float32).at[strand_number, stretch_shift].add(stretch_width)
    pass_tally = pass_tally - stretch_table[:, None, :]
    return jnp.cumsum(pass_tally, axis=2).astype(jnp.float32)


def draw_group_choice(key, part):
    block_total = MOE_TOKENS // TOK_DEV
    pool_size = GROUPS * CAP
    full_group = jax.random.randint(jax.random.fold_in(key, 31), (), 0, GROUPS).astype(jnp.int32)
    owner = (jnp.arange(pool_size, dtype=jnp.int32) // CAP).astype(jnp.int32)

    def one_block(block_index):
        block_key = jax.random.fold_in(key, 1000 + block_index)
        ranked = jax.random.permutation(jax.random.fold_in(block_key, 1), pool_size).astype(jnp.int32)
        priority = jnp.where(owner == full_group, ranked - pool_size, ranked)
        picked = owner[jnp.argsort(priority)[:TOK_DEV]]
        shuffle = jax.random.permutation(jax.random.fold_in(block_key, 2), TOK_DEV)
        return picked[shuffle]
    return jax.vmap(one_block)(jnp.arange(block_total, dtype=jnp.int32)).reshape(MOE_TOKENS).astype(jnp.int32)


def steps_of(stream_key, extent, pieces, smallest, high):
    gain, own = 1.0, jax.random.fold_in(stream_key, 6)
    for dim, blocks in pieces:
        draws = jnp.exp(jax.random.uniform(jax.random.fold_in(own, dim), (blocks,), jnp.float32, smallest / len(pieces), high / len(pieces)))
        gain = gain * jnp.repeat(draws, extent[dim] // blocks).reshape([-1 if axis == dim else 1 for axis in range(len(extent))])
    return gain


def gaussian(rng, dims, scale, most, shards=(), kind=jnp.bfloat16):
    factor_of = steps_of(rng, dims, shards, -0.22, 0.18) if shards else 1.0
    drawn = jax.random.normal(rng, dims, jnp.float32) * scale * factor_of
    return jnp.minimum(jnp.maximum(drawn, -most), most).astype(kind)


def setup_inputs(seed: int = 0) -> dict:
    streams_of = jax.random.split(jax.random.key(seed), 13)
    queries = draw_queries(jax.random.fold_in(streams_of[12], 71), 0)
    key_vectors = draw_key_vectors(jax.random.fold_in(streams_of[12], 71), 0)
    value_vectors = gaussian(streams_of[2], (STRAND_TOTAL, HD, STRAND_SPAN), 2.0, 12.0, ((1, 16), (2, 16)))
    cumulative_gate = draw_cumulative_gate(jax.random.fold_in(streams_of[12], 71), 0)
    expert_input = gaussian(streams_of[4], (MOE_TOKENS, D), 1.0, 6.0, ((0, 256),))
    norm_gain = jnp.clip(1.0 + 0.18 * jax.random.normal(streams_of[5], (D,), jnp.float32), 0.1, 1.9)
    group_choice = draw_group_choice(jax.random.fold_in(streams_of[12], 71), 0)
    group_weight = jnp.clip(jnp.exp(math.log(1.0) - 1.2039728 * jax.random.uniform(streams_of[7], (MOE_TOKENS,), jnp.float32) ** steps_of(streams_of[7], (MOE_TOKENS,), ((0, 256),), -0.2, 0.2)), 0.3, 1.0)
    expert_logits = gaussian(streams_of[8], (MOE_TOKENS, EPG), 1.5, 6.0, ((0, 256),), jnp.float32)
    gate_weight = gaussian(streams_of[9], (EXPERTS, FE, D), D ** -0.5, 0.125, ((0, 16), (1, 16)))
    up_weight = gaussian(streams_of[10], (EXPERTS, FE, D), D ** -0.5, 0.125, ((0, 16), (1, 16)))
    down_weight = gaussian(streams_of[11], (EXPERTS, FE, D), (FE // 4) ** -0.5, 0.25, ((0, 16), (1, 16)))
    return {"queries": queries, "key_vectors": key_vectors, "value_vectors": value_vectors, "cumulative_gate": cumulative_gate, "expert_input": expert_input, "norm_gain": norm_gain, "group_choice": group_choice, "group_weight": group_weight, "expert_logits": expert_logits, "gate_weight": gate_weight, "up_weight": up_weight, "down_weight": down_weight}


neg_fill = -1e+30
norm_eps = 1e-06

def head_attention(queries, key_vectors, value_vectors, cumulative_gate):
    query_rows = jnp.transpose(queries, (0, 2, 1))
    key_rows = jnp.transpose(key_vectors, (0, 2, 1))
    value_rows = jnp.transpose(value_vectors, (0, 2, 1))
    block_len = min(512, STRAND_SPAN)
    block_count = STRAND_SPAN // block_len
    score_scale = 1.0 / math.sqrt(HEAD)
    zero_index = jnp.zeros((), jnp.int32)
    key_positions = jnp.arange(STRAND_SPAN, dtype=jnp.int32)

    def one_pair(pair_index):
        strand_number = (pair_index // HEADS).astype(jnp.int32)
        head_index = (pair_index % HEADS).astype(jnp.int32)
        column = (head_index * HEAD).astype(jnp.int32)
        query_head = lax.dynamic_slice(query_rows, (strand_number, zero_index, column), (1, STRAND_SPAN, HEAD))[0]
        key_head = lax.dynamic_slice(key_rows, (strand_number, zero_index, column), (1, STRAND_SPAN, HEAD))[0]
        value_head = lax.dynamic_slice(value_rows, (strand_number, zero_index, column), (1, STRAND_SPAN, HEAD))[0]
        gate_head = lax.dynamic_slice(cumulative_gate, (strand_number, head_index, zero_index), (1, 1, STRAND_SPAN))[0, 0]

        def one_block(block_index):
            block_start = (block_index * block_len).astype(jnp.int32)
            query_block = lax.dynamic_slice_in_dim(query_head, block_start, block_len, 0)
            query_gate = lax.dynamic_slice_in_dim(gate_head, block_start, block_len, 0)
            scores = jnp.dot(query_block, key_head.T, preferred_element_type=jnp.float32) * score_scale
            scores = scores + (query_gate[:, None] - gate_head[None, :])
            query_positions = block_start + jnp.arange(block_len, dtype=jnp.int32)
            allowed = key_positions[None, :] <= query_positions[:, None]
            scores = jnp.where(allowed, scores, neg_fill)
            peak = lax.optimization_barrier(jnp.max(scores, axis=1, keepdims=True))
            expo = jnp.where(allowed, jnp.exp(scores - peak), 0.0)
            total = lax.optimization_barrier(jnp.sum(expo, axis=1, keepdims=True))
            mixed = jnp.dot(expo.astype(jnp.bfloat16), value_head, preferred_element_type=jnp.float32) / total
            return mixed.astype(jnp.bfloat16)
        return lax.map(one_block, jnp.arange(block_count, dtype=jnp.int32)).reshape(STRAND_SPAN, HEAD)
    heads_out = lax.map(one_pair, jnp.arange(STRAND_TOTAL * HEADS, dtype=jnp.int32))
    heads_out = heads_out.reshape(STRAND_TOTAL, HEADS, STRAND_SPAN, HEAD)
    return jnp.transpose(heads_out, (0, 1, 3, 2)).reshape(STRAND_TOTAL, HD, STRAND_SPAN)

def expert_mixture(expert_input, norm_gain, group_choice, group_weight, expert_logits, gate_weight, up_weight, down_weight):
    token_float = expert_input.astype(jnp.float32)
    normed = (token_float * lax.rsqrt(lax.optimization_barrier(jnp.mean(token_float * token_float, axis=1, keepdims=True)) + norm_eps) * norm_gain).astype(jnp.bfloat16)
    routing = (group_weight[:, None] * jax.nn.softmax(expert_logits, axis=1)).astype(jnp.bfloat16)
    block_total = MOE_TOKENS // TOK_DEV
    chosen = group_choice.reshape(block_total, TOK_DEV)
    member = (chosen[:, :, None] == jnp.arange(GROUPS, dtype=jnp.int32)[None, None, :]).astype(jnp.int32)
    before = jnp.cumsum(member, axis=1) - member
    slot_index = lax.optimization_barrier(jnp.sum(before * member, axis=2))
    block_ids = jnp.arange(block_total, dtype=jnp.int32)[:, None]
    flat_slot = ((chosen * block_total + block_ids) * CAP + slot_index).reshape(MOE_TOKENS).astype(jnp.int32)
    row_total = block_total * CAP
    row_buffer = jnp.zeros((GROUPS * row_total, D), jnp.bfloat16).at[flat_slot].set(normed).reshape(GROUPS, row_total, D)
    route_buffer = jnp.zeros((GROUPS * row_total, EPG), jnp.bfloat16).at[flat_slot].set(routing).reshape(GROUPS, row_total, EPG)
    hidden_width = FE // N_TP

    def one_group(group_index):
        group_rows = lax.optimization_barrier(row_buffer[group_index]).astype(jnp.float32)
        group_route = lax.optimization_barrier(route_buffer[group_index]).astype(jnp.float32)
        first_expert = (group_index * EPG).astype(jnp.int32)
        gate_block = lax.dynamic_slice_in_dim(gate_weight, first_expert, EPG, 0).astype(jnp.float32)
        up_block = lax.dynamic_slice_in_dim(up_weight, first_expert, EPG, 0).astype(jnp.float32)
        down_block = lax.dynamic_slice_in_dim(down_weight, first_expert, EPG, 0).astype(jnp.float32)
        gate_act = jnp.einsum('rd,efd->ref', group_rows, gate_block)
        up_act = jnp.einsum('rd,efd->ref', group_rows, up_block)
        hidden = (jax.nn.silu(gate_act) * up_act * group_route[:, :, None]).astype(jnp.bfloat16)
        hidden = lax.optimization_barrier(hidden).astype(jnp.float32).reshape(row_total, EPG, N_TP, hidden_width)
        partial_sums = jnp.einsum('rejf,ejfd->rjd', hidden, down_block.reshape(EPG, N_TP, hidden_width, D))
        partial_sums = lax.optimization_barrier(partial_sums.astype(jnp.bfloat16)).astype(jnp.float32)
        return lax.optimization_barrier(jnp.sum(partial_sums, axis=1)).astype(jnp.bfloat16)
    group_out = lax.map(one_group, jnp.arange(GROUPS, dtype=jnp.int32))
    return group_out.reshape(GROUPS * row_total, D)[flat_slot]

def reference(queries, key_vectors, value_vectors, cumulative_gate, expert_input, norm_gain, group_choice, group_weight, expert_logits, gate_weight, up_weight, down_weight):
    attention = head_attention(queries, key_vectors, value_vectors, cumulative_gate)
    expert_output = expert_mixture(expert_input, norm_gain, group_choice, group_weight, expert_logits, gate_weight, up_weight, down_weight)
    return (attention, expert_output)
```

```python
import jax
import jax.numpy as jnp
from jax import lax
from jax.experimental import pallas as pl
from jax.experimental.pallas import tpu as pltpu
from jax.sharding import PartitionSpec as P

MESH = pl.DeviceIdType.MESH
F32 = jnp.float32
BF16 = jnp.bfloat16

NX, NY, NZ = 4, 4, 8
NEP = NX * NY
SEG = 1024
HEAD = 64
TOK = 128
DIM = 2048
CAP = 10
QB = 8
CW = DIM // QB
HALF = 8 * CAP
STACK = QB * HALF
PAGE = QB * CAP
RT = 16
NEG = -1e30
EPS = 1e-6
ACC = 80


def dot(a, b, ca=1, cb=0):
    return lax.dot_general(a, b, (((ca,), (cb,)), ((), ())), preferred_element_type=F32)


def iota(shape, dim):
    return lax.broadcasted_iota(jnp.int32, shape, dim)


def iota_f(shape, dim):
    return iota(shape, dim).astype(F32)


def onehot(cond):
    return jnp.where(cond, 1.0, 0.0).astype(BF16)


def rem(a, n):
    return lax.rem(a, jnp.int32(n))


def div(a, n):
    return lax.div(a, jnp.int32(n))


def stacked_of_paged(r):
    src = jnp.floor((r + 0.5) * (1.0 / PAGE))
    left = r - PAGE * src
    blk = jnp.floor((left + 0.5) * (1.0 / CAP))
    slot = left - CAP * blk
    return HALF * blk + CAP * src + slot


def body(
    q_hbm, k_hbm, v_hbm, gate_ref, x_ref, gain_ref, small_ref, wg_hbm, wu_hbm, wd_hbm,
    att_ref, out_ref,
    wg, wu, wd, pages, arr, retp, ret, perm_in, perm_out, mh, pt,
    gown, gsib, pown, tosib, sibr, rsr, kraw, vaug, qaug, kt, acc, orecv,
    w_sem, l_sem, a_s, a_r, b_s, b_r, ag_s, ag_r, dr_s, dr_r, dp_s, dp_r, rs_s, rs_r,
    t_s, t_r, o_s, o_r,
):
    ep = lax.axis_index("ep")
    tp = lax.axis_index("tp")
    y, x = div(ep, NX), rem(ep, NX)
    z, core = div(tp, 2), rem(tp, 2)
    sib = z * 2 + (1 - core)
    up = rem(z + 1, NZ) * 2 + core
    down = rem(z + NZ - 1, NZ) * 2 + core
    ring = (up, down)

    def remote(src, dst, ss, rs, e, t):
        return pltpu.make_async_remote_copy(
            src_ref=src, dst_ref=dst, send_sem=ss, recv_sem=rs,
            device_id=(e, t), device_id_type=MESH,
        )

    barrier = pltpu.get_barrier_semaphore()

    @pl.loop(1, NEP)
    def _(d):
        pl.semaphore_signal(barrier, inc=1, device_id=(rem(ep + d, NEP), tp), device_id_type=MESH)

    for t in (up, down, sib):
        pl.semaphore_signal(barrier, inc=1, device_id=(ep, t), device_id_type=MESH)

    w_copies = [
        pltpu.make_async_copy(src, dst, w_sem.at[n])
        for n, (src, dst) in enumerate(((wg_hbm, wg), (wu_hbm, wu), (wd_hbm, wd)))
    ]
    for c in w_copies:
        c.start()
    q_own = (y, 4 + x)
    kv_own = (x, 4 + y)
    l_copies = []
    for s in range(2):
        l_copies += [
            pltpu.make_async_copy(q_hbm.at[s], qaug.at[q_own[s], pl.ds(0, HEAD)], l_sem.at[3 * s]),
            pltpu.make_async_copy(k_hbm.at[s], kraw.at[kv_own[s]], l_sem.at[3 * s + 1]),
            pltpu.make_async_copy(v_hbm.at[s], vaug.at[kv_own[s], pl.ds(0, HEAD)], l_sem.at[3 * s + 2]),
        ]
    for c in l_copies:
        c.start()

    tok = x_ref[...].astype(F32)
    normed = (
        tok * lax.rsqrt(jnp.mean(tok * tok, axis=1, keepdims=True) + EPS) * gain_ref[...]
    ).astype(BF16)
    l0, l1 = small_ref[0:1, :], small_ref[1:2, :]
    gw, gc = small_ref[2:3, :], small_ref[3:4, :]
    top = jnp.maximum(l0, l1)
    e0, e1 = jnp.exp(l0 - top), jnp.exp(l1 - top)
    r0 = (gw * (e0 / (e0 + e1))).astype(BF16).astype(F32)
    r1 = (gw * (e1 / (e0 + e1))).astype(BF16).astype(F32)
    member = jnp.where(iota_f((NEP, TOK), 0) == gc, 1.0, 0.0)
    earlier = onehot(iota((TOK, TOK), 0) < iota((TOK, TOK), 1))
    before = dot(member.astype(BF16), earlier)
    slot = jnp.sum(before * member, axis=0, keepdims=True)
    flat = gc * PAGE + slot
    rows_p = iota_f((NEP * PAGE, TOK), 0)
    packed = jnp.zeros((NEP * PAGE, CW), F32)
    for b in range(0, QB, 2):
        put = jnp.concatenate(
            [onehot(rows_p == flat + CAP * b), onehot(rows_p == flat + CAP * (b + 1))], axis=1
        )
        cols = jnp.concatenate(
            [normed[:, b * CW:(b + 1) * CW], normed[:, (b + 1) * CW:(b + 2) * CW]], axis=0
        )
        packed = packed + dot(put, cols)
    packed = packed.astype(BF16)
    eye = iota((TOK, TOK), 0) == iota((TOK, TOK), 1)
    ones = jnp.ones((TOK, TOK), BF16)
    col_g = dot(jnp.where(eye, gc, 0.0).astype(BF16), ones)
    col_s = dot(jnp.where(eye, slot, 0.0).astype(BF16), ones)
    flat10 = col_g * CAP + col_s
    place10 = onehot(iota_f((TOK, CW), 1) == jnp.concatenate([flat10, flat10], axis=1))
    e_rows = iota((RT, TOK), 0)
    rr = jnp.where(e_rows == 0, r0, jnp.where(e_rows == 1, r1, 0.0)).astype(BF16)
    rt_all = dot(rr, place10).astype(BF16)
    for g in range(NEP):
        pages[g, 0:PAGE, :] = packed[g * PAGE:(g + 1) * PAGE, :]
        pages[g, PAGE:PAGE + RT, :] = rt_all

    pl.semaphore_wait(barrier, NEP + 2)

    def a2a(e):
        return remote(pages.at[e], arr.at[ep], a_s.at[e], a_r.at[ep], e, tp)

    @pl.loop(1, NEP)
    def _(d):
        a2a(rem(ep + d, NEP)).start()

    arr[ep] = pages[ep]

    def along(axis, d):
        if axis == 0:
            return y * NX + rem(x + d, NX)
        return rem(y + d, NY) * NX + x

    def spread(s, d):
        kv_axis, q_axis = s, 1 - s
        e_kv, e_q = along(kv_axis, d), along(q_axis, d)
        return (
            remote(k_hbm.at[s], kraw.at[kv_own[s]], t_s.at[s, 0, d], t_r.at[0, kv_own[s]], e_kv, tp),
            remote(v_hbm.at[s], vaug.at[kv_own[s], pl.ds(0, HEAD)], t_s.at[s, 1, d],
                   t_r.at[1, kv_own[s]], e_kv, tp),
            remote(q_hbm.at[s], qaug.at[q_own[s], pl.ds(0, HEAD)], t_s.at[s, 2, d],
                   t_r.at[2, q_own[s]], e_q, tp),
        )

    for s in range(2):
        for d in range(1, 4):
            for c in spread(s, d):
                c.start()

    sq = (STACK, STACK)
    perm_in[...] = onehot(iota_f(sq, 0) == stacked_of_paged(iota_f(sq, 1)))
    perm_out[...] = onehot(iota_f(sq, 1) == stacked_of_paged(iota_f(sq, 0)))
    epf = ep.astype(F32)
    for sl in range(8):
        off = iota_f((CW, CW), 0) - CAP * epf
        hit = (iota_f((CW, CW), 1) - CAP * sl == off) & (off >= 0.0) & (off < CAP)
        mh[sl * CW:(sl + 1) * CW, :] = onehot(hit)
    col_flat = col_g * PAGE + col_s
    wide = jnp.concatenate([col_flat] * (NEP * PAGE // TOK), axis=1)
    lanes_p = iota_f((TOK, NEP * PAGE), 1)
    for b in range(QB):
        pt[b * TOK:(b + 1) * TOK, :] = onehot(lanes_p == wide + CAP * b)

    @pl.loop(0, 8)
    def _(n):
        qaug[n, HEAD:2 * HEAD, :] = onehot(iota((HEAD, SEG), 0) < 3)
        vaug[n, HEAD:ACC, :] = onehot(iota((ACC - HEAD, SEG), 0) < 1)
        acc[n, 0:72, :] = jnp.zeros((72, SEG), F32)
        acc[n, 72:ACC, :] = jnp.full((ACC - 72, SEG), NEG, F32)

    for h in range(2):
        rsr[h, 0] = jnp.zeros((STACK, CW), BF16)

    def ag(h, i):
        return remote(gown.at[h, i], gown.at[h, i + 1], ag_s.at[h, i], ag_r.at[h, i], ep, ring[h])

    def rows_to_sib(h, j):
        return remote(gown.at[h, j], gsib.at[h, j], dr_s.at[h, j], dr_r.at[h, j], ep, sib)

    def sums_to_sib(h, j):
        return remote(tosib.at[h, j], sibr.at[h, j], dp_s.at[h, j], dp_r.at[h, j], ep, sib)

    def rs(h, r):
        return remote(pown.at[h, r + 1], rsr.at[h, r + 1], rs_s.at[h, r], rs_r.at[h, r], ep, ring[h])

    for h in range(2):
        for sl in range(8):
            src = 8 * h + sl

            @pl.when(src != ep)
            def _():
                remote(pages.at[src], arr.at[src], a_s.at[src], a_r.at[src], src, tp).wait_recv()

        paged = jnp.concatenate([arr[8 * h + sl, 0:PAGE, :] for sl in range(8)], axis=0)
        rts = jnp.concatenate([arr[8 * h + sl, PAGE:PAGE + RT, :] for sl in range(8)], axis=1)
        gown[h, 0, 0:STACK, :] = dot(perm_in[...], paged).astype(BF16)
        gown[h, 0, STACK:STACK + RT, :] = dot(rts, mh[...]).astype(BF16)
        ag(h, 0).start()
        rows_to_sib(h, 0).start()

    for c in w_copies:
        c.wait()
    for c in l_copies:
        c.wait()

    def expert(i):
        j = rem(i + 1, NZ)
        pieces = (gown.at[0, j], gown.at[1, j], gsib.at[0, i], gsib.at[1, i])
        lhs = jnp.concatenate(
            [
                jnp.concatenate([p[b * HALF:(b + 1) * HALF, :] for b in range(QB)], axis=1)
                for p in pieces
            ],
            axis=0,
        )
        diag = iota((HALF, TOK), 0) == iota((HALF, TOK), 1)
        one = jnp.ones((TOK, TOK), BF16)
        scale = []
        for p in pieces:
            tile = p[STACK:STACK + RT, 0:TOK].astype(F32)
            scale.append(
                jnp.concatenate(
                    [dot(jnp.where(diag, tile[e:e + 1, :], 0.0).astype(BF16), one) for e in range(2)],
                    axis=1,
                )
            )
        scale = jnp.concatenate(scale, axis=0)
        gate = dot(lhs, wg[...], 1, 1)
        upv = dot(lhs, wu[...], 1, 1)
        hidden = (gate / (1.0 + jnp.exp(-gate)) * upv * scale).astype(BF16)
        outs = (pown.at[0, j], pown.at[1, j], tosib.at[0, i], tosib.at[1, i])
        for b in range(QB):
            prod = dot(hidden, wd[:, b * CW:(b + 1) * CW]).astype(BF16)
            for n, o in enumerate(outs):
                o[b * HALF:(b + 1) * HALF, :] = prod[n * HALF:(n + 1) * HALF, :]
        for h in range(2):
            sums_to_sib(h, i).start()

    def attention_ready():
        for s in range(2):
            for d in range(1, 4):
                kv = 4 * s + rem(kv_own[s] - 4 * s + d, 4)
                qs = 4 * s + rem(q_own[s] - 4 * s + d, 4)
                remote(k_hbm.at[s], kraw.at[kv], t_s.at[s, 0, d], t_r.at[0, kv], ep, sib).wait_recv()
                remote(v_hbm.at[s], vaug.at[kv, pl.ds(0, HEAD)], t_s.at[s, 1, d], t_r.at[1, kv], ep,
                       sib).wait_recv()
                remote(q_hbm.at[s], qaug.at[qs, pl.ds(0, HEAD)], t_s.at[s, 2, d], t_r.at[2, qs], ep,
                       sib).wait_recv()

        @pl.loop(0, 8)
        def _(n):
            s = div(n, 4)
            chunk = (1 - s) * (4 * y + n) + s * (x + 4 * (n - 4))
            g = gate_ref[s, :, pl.ds(pl.multiple_of(chunk * SEG, SEG), SEG)]
            d = g[:, SEG - 1:SEG] - g
            hi = d.astype(BF16).astype(F32)
            mid = (d - hi).astype(BF16).astype(F32)
            lo = d - hi - mid
            r = iota((8, SEG), 0)
            rows = jnp.where(r == 0, hi, jnp.where(r == 1, mid, jnp.where(r == 2, lo, 0.0)))
            feats = kraw[n].astype(F32) * 0.125
            full = jnp.concatenate([feats, rows, jnp.zeros((56, SEG), F32)], axis=0)
            kt[n] = full.T.astype(BF16)

    n_first = 4 * (3 - y) + x + 1

    def unit(b):
        s = (b >= n_first).astype(jnp.int32)
        u0 = b
        late0 = (u0 > x).astype(jnp.int32)
        t0 = late0 * (u0 - x - 1)
        k0 = y + late0 * (1 + div(t0, 4))
        m0 = late0 * rem(t0, 4) + (1 - late0) * u0
        d0 = (u0 == x).astype(jnp.int32)
        u1 = s * (b - n_first)
        late1 = (u1 >= 4 * y).astype(jnp.int32)
        k1 = late1 * y + (1 - late1) * div(u1, 4)
        m1 = late1 * (x + u1 - 4 * y) + (1 - late1) * rem(u1, 4)
        d1 = (u1 == 4 * y).astype(jnp.int32)
        qs = (1 - s) * k0 + s * (4 + m1)
        kv = (1 - s) * m0 + s * (4 + k1)
        qc = (1 - s) * (4 * k0 + x) + s * (4 * y + m1)
        kc = (1 - s) * (4 * y + m0) + s * (x + 4 * k1)
        slack = (1 - ((1 - s) * d0 + s * d1)) * (2 * SEG)
        qs, kv = rem(qs, 8), rem(kv, 8)
        qc, kc = rem(qc, NEP), rem(kc, NEP)
        ref_end = gate_ref[s, :, pl.ds(pl.multiple_of(kc * SEG + SEG - 128, 128), 128)][:, 127:128]

        @pl.loop(0, SEG // 256)
        def _(c):
            at = pl.multiple_of(c * 256, 256)
            lanes = pl.ds(at, 256)
            sc = dot(kt[kv], qaug[qs, :, lanes])
            keep = iota((SEG, 256), 0) <= iota((SEG, 256), 1) + (at + slack)
            sc = jnp.where(keep, sc, NEG)
            peak = jnp.max(sc, axis=0, keepdims=True)
            w = jnp.exp(sc - peak).astype(BF16)
            o = dot(vaug[kv], w)
            gq = gate_ref[s, :, pl.ds(pl.multiple_of(qc * SEG + at, 256), 256)]
            peak = peak + (gq - ref_end)
            old = acc[qs, 72:73, lanes]
            new = jnp.maximum(old, peak)
            acc[qs, 0:72, lanes] = acc[qs, 0:72, lanes] * jnp.exp(old - new) + o[0:72] * jnp.exp(peak - new)
            acc[qs, 72:ACC, lanes] = jnp.broadcast_to(new, (ACC - 72, 256))

    def give(s, d):
        e = along(1 - s, d)
        mine = q_own[s] - 4 * s
        theirs = 4 * s + rem(mine + d, 4)
        return remote(acc.at[theirs], orecv.at[s, mine], o_s.at[s, d], o_r.at[s, mine], e, tp)

    UNITS = 17
    PER = 4

    @pl.loop(0, NZ)
    def _(i):
        @pl.when(i < NZ - 1)
        def _():
            for h in range(2):
                ag(h, i).wait_recv()

                @pl.when(i < NZ - 2)
                def _():
                    ag(h, i + 1).start()

                rows_to_sib(h, i + 1).start()

        for h in range(2):
            rows_to_sib(h, i).wait_recv()
        expert(i)

        @pl.when(i == 1)
        def _():
            attention_ready()

        first = jnp.maximum(PER * (i - 1), 0)
        last = jnp.minimum(PER * i, UNITS)

        @pl.loop(first, last)
        def _(b):
            unit(b)

        @pl.when(i == 6)
        def _():
            for s in range(2):
                for d in range(1, 4):
                    give(s, d).start()

        @pl.when(i >= 1)
        def _():
            r = i - 1
            for h in range(2):
                sums_to_sib(h, i).wait_recv()

                @pl.when(r >= 1)
                def _():
                    rs(h, r - 1).wait_recv()

                pown[h, i] = (
                    pown[h, i].astype(F32) + sibr[h, i].astype(F32) + rsr[h, r].astype(F32)
                ).astype(BF16)
                rs(h, r).start()

    def back(e):
        return remote(retp.at[e], ret.at[ep], b_s.at[e], b_r.at[ep], e, tp)

    for h in range(2):
        sums_to_sib(h, 0).wait_recv()
        rs(h, NZ - 2).wait_recv()
        total = (
            pown[h, 0].astype(F32) + sibr[h, 0].astype(F32) + rsr[h, NZ - 1].astype(F32)
        ).astype(BF16)
        paged = dot(perm_out[...], total).astype(BF16)
        for sl in range(8):
            src = 8 * h + sl
            retp[src] = paged[sl * PAGE:(sl + 1) * PAGE, :]

            @pl.when(src != ep)
            def _():
                back(src).start()

    ret[ep] = retp[ep]

    for s in range(2):
        mine = q_own[s] - 4 * s
        for d in range(1, 4):
            slot_d = rem(mine + d, 4)
            remote(acc.at[0], orecv.at[s, slot_d], o_s.at[s, d], o_r.at[s, slot_d], ep, sib).wait_recv()
        for c in range(SEG // 256):
            lanes = slice(c * 256, (c + 1) * 256)
            parts = [acc.at[q_own[s]]] + [orecv.at[s, rem(mine + d, 4)] for d in range(1, 4)]
            peaks = [p[72:73, lanes] for p in parts]
            top = jnp.maximum(jnp.maximum(peaks[0], peaks[1]), jnp.maximum(peaks[2], peaks[3]))
            mix = sum(p[0:72, lanes] * jnp.exp(m - top) for p, m in zip(parts, peaks))
            att_ref[s, :, lanes] = (mix[0:HEAD] / mix[HEAD:HEAD + 1]).astype(BF16)

    for src in range(NEP):
        @pl.when(src != ep)
        def _():
            remote(retp.at[src], ret.at[src], b_s.at[src], b_r.at[src], src, tp).wait_recv()

    back_rows = jnp.concatenate([ret[g] for g in range(NEP)], axis=0)
    placed = dot(pt[...], back_rows).astype(BF16)
    for b in range(QB):
        out_ref[:, b * CW:(b + 1) * CW] = placed[b * TOK:(b + 1) * TOK, :]

    @pl.loop(1, NEP)
    def _(d):
        e = rem(ep + d, NEP)
        a2a(e).wait_send()
        back(e).wait_send()

    for s in range(2):
        for d in range(1, 4):
            for c in spread(s, d):
                c.wait_send()
            give(s, d).wait_send()
    for h in range(2):
        @pl.loop(0, NZ - 1)
        def _(i):
            ag(h, i).wait_send()
            rs(h, i).wait_send()

        @pl.loop(0, NZ)
        def _(i):
            rows_to_sib(h, i).wait_send()
            sums_to_sib(h, i).wait_send()


def local(
    queries, key_vectors, value_vectors, cumulative_gate, expert_input, norm_gain,
    group_choice, group_weight, expert_logits, gate_weight, up_weight, down_weight,
):
    small = jnp.concatenate(
        [expert_logits.T, group_weight[None], group_choice.astype(F32)[None], jnp.zeros((4, TOK), F32)],
        axis=0,
    )
    vmem = pl.BlockSpec(memory_space=pltpu.VMEM)
    hbm = pl.BlockSpec(memory_space=pltpu.HBM)
    dma = pltpu.SemaphoreType.DMA
    v = pltpu.VMEM
    scratch = [
        v((256, DIM), BF16), v((256, DIM), BF16), v((256, DIM), BF16),
        v((NEP, PAGE + RT, CW), BF16), v((NEP, PAGE + RT, CW), BF16),
        v((NEP, PAGE, CW), BF16), v((NEP, PAGE, CW), BF16),
        v((STACK, STACK), BF16), v((STACK, STACK), BF16),
        v((8 * CW, CW), BF16), v((QB * TOK, NEP * PAGE), BF16),
        v((2, NZ, STACK + RT, CW), BF16), v((2, NZ, STACK + RT, CW), BF16),
        v((2, NZ, STACK, CW), BF16), v((2, NZ, STACK, CW), BF16), v((2, NZ, STACK, CW), BF16),
        v((2, NZ, STACK, CW), BF16),
        v((8, HEAD, SEG), BF16), v((8, ACC, SEG), BF16), v((8, 2 * HEAD, SEG), BF16),
        v((8, SEG, 2 * HEAD), BF16), v((8, ACC, SEG), F32), v((2, 4, ACC, SEG), F32),
        dma((3,)), dma((6,)), dma((NEP,)), dma((NEP,)), dma((NEP,)), dma((NEP,)),
        dma((2, NZ - 1)), dma((2, NZ - 1)), dma((2, NZ)), dma((2, NZ)), dma((2, NZ)), dma((2, NZ)),
        dma((2, NZ - 1)), dma((2, NZ - 1)), dma((2, 3, 4)), dma((3, 8)), dma((2, 4)), dma((2, 4)),
    ]
    return pl.pallas_call(
        body,
        out_shape=(
            jax.ShapeDtypeStruct(queries.shape, BF16),
            jax.ShapeDtypeStruct(expert_input.shape, BF16),
        ),
        in_specs=[hbm, hbm, hbm, vmem, vmem, vmem, vmem, hbm, hbm, hbm],
        out_specs=(vmem, vmem),
        scratch_shapes=scratch,
        compiler_params=pltpu.CompilerParams(
            collective_id=0, has_side_effects=True, vmem_limit_bytes=67043328
        ),
    )(
        queries, key_vectors, value_vectors, cumulative_gate, expert_input, norm_gain[None],
        small, gate_weight.reshape(256, DIM), up_weight.reshape(256, DIM), down_weight.reshape(256, DIM),
    )


def solution(mesh):
    return jax.shard_map(
        local,
        mesh=mesh,
        in_specs=(
            P(None, "tp", "ep"),
            P(None, "tp", "ep"),
            P(None, "tp", "ep"),
            P(None, "tp", None),
            P(("ep", "tp"), None),
            P(),
            P(("ep", "tp")),
            P(("ep", "tp")),
            P(("ep", "tp"), None),
            P("ep", "tp", None),
            P("ep", "tp", None),
            P("ep", "tp", None),
        ),
        out_specs=(P(None, "tp", "ep"), P(("ep", "tp"), None)),
        check_vma=False,
    )
```

```python
import jax
import jax.numpy as jnp
from jax import lax
from jax.experimental import pallas as pl
from jax.experimental.pallas import tpu as pltpu
from jax.sharding import PartitionSpec as P

MESH = pl.DeviceIdType.MESH
F32 = jnp.float32
BF16 = jnp.bfloat16

NX, NY, NZ = 4, 4, 8
NEP = NX * NY
SEG = 1024
HEAD = 64
TOK = 128
DIM = 2048
CAP = 10
QB = 16
CW = DIM // QB
HALF = 8 * CAP
STACK = QB * HALF
NU = 4
UB = QB // NU
SUB = STACK // NU
SPAGE = UB * CAP
BIG = STACK // 2
RT = 8
NEG = -1e30
TILE = 512
EPS = 1e-6
ACC = 80


def dot(a, b, ca=1, cb=0):
    return lax.dot_general(a, b, (((ca,), (cb,)), ((), ())), preferred_element_type=F32)


def iota(shape, dim):
    return lax.broadcasted_iota(jnp.int32, shape, dim)


def iota_f(shape, dim):
    return iota(shape, dim).astype(F32)


def onehot(cond):
    return jnp.where(cond, 1.0, 0.0).astype(BF16)


def rem(a, n):
    return lax.rem(a, jnp.int32(n))


def div(a, n):
    return lax.div(a, jnp.int32(n))


def stacked_of_paged(r):
    src = jnp.floor((r + 0.5) * (1.0 / SPAGE))
    left = r - SPAGE * src
    blk = jnp.floor((left + 0.5) * (1.0 / CAP))
    slot = left - CAP * blk
    return HALF * blk + CAP * src + slot


def body(
    q_hbm, k_hbm, v_hbm, gate_hbm, x_hbm, gain_hbm, lg_hbm, gw_hbm, gc_hbm, wg_hbm, wu_hbm, wd_hbm,
    att_ref, out_ref,
    gate_ref, x_ref, gain_ref, lg_ref, gw_ref, gc_ref, wg, wu, wd, pages, arr, pages_rt, arr_rt, retp, ret, perm_in, perm_out, mh, pt,
    gown, gsib, pown, tosib, sibr, rsr, kraw, vaug, qaug, kt, acc, orecv,
    i_sem, w_sem, l_sem, a_s, a_r, art_s, art_r, b_s, b_r, ag_s, ag_r, dr_s, dr_r, dp_s, dp_r, rs_s, rs_r, rl_r,
    t_s, t_r, o_s, o_r,
):
    ep = lax.axis_index("ep")
    tp = lax.axis_index("tp")
    y, x = div(ep, NX), rem(ep, NX)
    z, core = div(tp, 2), rem(tp, 2)
    sib = z * 2 + (1 - core)
    up = rem(z + 1, NZ) * 2 + core
    down = rem(z + NZ - 1, NZ) * 2 + core
    ring = (up, down)

    def remote(src, dst, ss, rs, e, t):
        return pltpu.make_async_remote_copy(
            src_ref=src, dst_ref=dst, send_sem=ss, recv_sem=rs,
            device_id=(e, t), device_id_type=MESH,
        )

    i_copies = [
        pltpu.make_async_copy(src, dst, i_sem.at[n])
        for n, (src, dst) in enumerate((
            (x_hbm, x_ref), (gain_hbm, gain_ref), (lg_hbm, lg_ref), (gw_hbm, gw_ref), (gc_hbm, gc_ref),
            (gate_hbm, gate_ref),
        ))
    ]
    for c in i_copies[:5]:
        c.start()
    barrier = pltpu.get_barrier_semaphore()

    @pl.loop(1, NEP)
    def _(d):
        pl.semaphore_signal(barrier, inc=1, device_id=(rem(ep + d, NEP), tp), device_id_type=MESH)

    for t in (up, down, sib):
        pl.semaphore_signal(barrier, inc=1, device_id=(ep, t), device_id_type=MESH)

    w_copies = [
        pltpu.make_async_copy(src, dst, w_sem.at[n])
        for n, (src, dst) in enumerate(((wg_hbm, wg), (wu_hbm, wu), (wd_hbm, wd)))
    ]
    for c in w_copies:
        c.start()
    q_own = (y, 4 + x)
    kv_own = (x, 4 + y)
    l_copies = []
    for s in range(2):
        l_copies += [
            pltpu.make_async_copy(q_hbm.at[s], qaug.at[q_own[s], pl.ds(0, HEAD)], l_sem.at[3 * s]),
            pltpu.make_async_copy(k_hbm.at[s], kraw.at[kv_own[s]], l_sem.at[3 * s + 1]),
            pltpu.make_async_copy(v_hbm.at[s], vaug.at[kv_own[s], pl.ds(0, HEAD)], l_sem.at[3 * s + 2]),
        ]
    for c in l_copies:
        c.start()

    i_copies[5].start()

    n_pack = NEP * SPAGE
    r = iota_f((n_pack, n_pack), 0)
    grp = jnp.floor((r + 0.5) * (1.0 / SPAGE))
    left = r - SPAGE * grp
    blk = jnp.floor((left + 0.5) * (1.0 / CAP))
    perm_pack = onehot(iota_f((n_pack, n_pack), 1) == NEP * CAP * blk + CAP * grp + left - CAP * blk)
    for c in i_copies[:5]:
        c.wait()
    tok = x_ref[...].astype(F32)
    normed = (
        tok * lax.rsqrt(jnp.mean(tok * tok, axis=1, keepdims=True) + EPS) * gain_ref[...]
    ).astype(BF16)
    l0, l1 = lg_ref[0:1, :], lg_ref[1:2, :]
    gw, gc = gw_ref[...], gc_ref[...].astype(F32)
    top = jnp.maximum(l0, l1)
    e0, e1 = jnp.exp(l0 - top), jnp.exp(l1 - top)
    r0 = (gw * (e0 / (e0 + e1))).astype(BF16).astype(F32)
    r1 = (gw * (e1 / (e0 + e1))).astype(BF16).astype(F32)
    member = jnp.where(iota_f((NEP, TOK), 0) == gc, 1.0, 0.0)
    earlier = onehot(iota((TOK, TOK), 0) < iota((TOK, TOK), 1))
    before = dot(member.astype(BF16), earlier)
    slot = jnp.sum(before * member, axis=0, keepdims=True)
    places = onehot(iota_f((NEP * CAP, TOK), 0) == gc * CAP + slot)
    outgoing = dot(places, normed).astype(BF16)
    for w in range(0, NU, 2):
        blocks = [
            jnp.concatenate(
                [outgoing[:, b * CW:(b + 1) * CW] for b in range(UB * u, UB * (u + 1))], axis=0
            )
            for u in (w, w + 1)
        ]
        packed = dot(perm_pack, jnp.concatenate(blocks, axis=1)).astype(BF16)
        for g in range(NEP):
            for n in range(2):
                pages[w + n, g] = packed[g * SPAGE:(g + 1) * SPAGE, n * CW:(n + 1) * CW]
    eye = iota((TOK, TOK), 0) == iota((TOK, TOK), 1)
    ones = jnp.ones((TOK, TOK), BF16)
    col_g = dot(jnp.where(eye, gc, 0.0).astype(BF16), ones)
    col_s = dot(jnp.where(eye, slot, 0.0).astype(BF16), ones)
    e_rows = iota((16, TOK), 0)
    rr = jnp.where(e_rows == 0, r0, jnp.where(e_rows == 1, r1, 0.0)).astype(BF16)
    lanes_g = jnp.concatenate([col_g * TOK + col_s] * NEP, axis=1)
    rt_all = dot(rr, onehot(iota_f((TOK, NEP * TOK), 1) == lanes_g)).astype(BF16)
    for g in range(NEP):
        pages_rt[g] = rt_all[0:RT, g * TOK:(g + 1) * TOK]

    with jax.named_scope("entry"):
        pl.semaphore_wait(barrier, NEP + 2)

    def a2a(e, u):
        return remote(pages.at[u, e], arr.at[u, ep], a_s, a_r.at[u, div(ep, 8)], e, tp)

    def a2a_rt(e):
        return remote(pages_rt.at[e], arr_rt.at[ep], art_s, art_r, e, tp)

    for u in range(NU):
        @pl.loop(1, NEP)
        def _(d):
            a2a(rem(ep + d, NEP), u).start()

    @pl.loop(1, NEP)
    def _(d):
        a2a_rt(rem(ep + d, NEP)).start()

    for u in range(NU):
        arr[u, ep] = pages[u, ep]
    arr_rt[ep] = pages_rt[ep]

    def along(axis, d):
        if axis == 0:
            return y * NX + rem(x + d, NX)
        return rem(y + d, NY) * NX + x

    def spread(s, d):
        kv_axis, q_axis = s, 1 - s
        e_kv, e_q = along(kv_axis, d), along(q_axis, d)
        return (
            remote(k_hbm.at[s], kraw.at[kv_own[s]], t_s.at[s, 0], t_r.at[s, 0], e_kv, tp),
            remote(v_hbm.at[s], vaug.at[kv_own[s], pl.ds(0, HEAD)], t_s.at[s, 1],
                   t_r.at[s, 1], e_kv, tp),
            remote(q_hbm.at[s], qaug.at[q_own[s], pl.ds(0, HEAD)], t_s.at[s, 2],
                   t_r.at[s, 2], e_q, tp),
        )

    sq = (SUB, SUB)
    perm_in[...] = onehot(iota_f(sq, 0) == stacked_of_paged(iota_f(sq, 1)))
    perm_out[...] = onehot(iota_f(sq, 1) == stacked_of_paged(iota_f(sq, 0)))
    for sl in range(8):
        left = iota((TOK, TOK), 0)
        hit = (iota((TOK, TOK), 1) - CAP * sl == left) & (left < CAP)
        mh[sl * TOK:(sl + 1) * TOK, :] = onehot(hit)
    wide = jnp.concatenate([col_g * SPAGE + col_s] * (NEP * SPAGE // TOK), axis=1)
    lanes_p = iota_f((TOK, NEP * SPAGE), 1)
    for b in range(UB):
        pt[b * TOK:(b + 1) * TOK, :] = onehot(lanes_p == wide + CAP * b)

    @pl.loop(0, 8)
    def _(n):
        qaug[n, HEAD:2 * HEAD, :] = onehot(iota((HEAD, SEG), 0) < 3)
        vaug[n, HEAD:ACC, :] = onehot(iota((ACC - HEAD, SEG), 0) < 1)
        acc[n, 0:72, :] = jnp.zeros((72, SEG), F32)
        acc[n, 72:ACC, :] = jnp.full((ACC - 72, SEG), NEG, F32)

    for h in range(2):
        rsr[h, 0] = jnp.zeros((STACK, CW), BF16)

    def ag(h, c, i):
        rows = pl.ds(BIG * c, BIG + RT * c)
        return remote(
            gown.at[h, i, rows], gown.at[h, i + 1, rows], ag_s.at[h], ag_r.at[h, c, i], ep, ring[h]
        )

    def ag_first(h, u):
        rows = pl.ds(SUB * u, SUB + RT * (u == NU - 1))
        return remote(
            gown.at[h, 0, rows], gown.at[h, 1, rows], ag_s.at[h], ag_r.at[h, u // 2, 0], ep, ring[h]
        )

    def rows_to_sib(h, j):
        return remote(gown.at[h, j], gsib.at[h, j], dr_s.at[h], dr_r.at[j], ep, sib)

    def rows_from_sib(j):
        both = gsib.at[pl.ds(0, 2), j]
        return remote(both, both, dr_s.at[0], dr_r.at[j], ep, sib)

    def sums_to_sib(h, j):
        return remote(tosib.at[h, rem(j, 2)], sibr.at[h, j], dp_s.at[h, rem(j, 2)], dp_r.at[j], ep, sib)

    def sums_from_sib(j):
        both = sibr.at[pl.ds(0, 2), j]
        return remote(both, both, dp_s.at[0, 0], dp_r.at[j], ep, sib)

    def rs(h, c, r):
        rows = pl.ds(BIG * c, BIG)
        return remote(
            pown.at[h, r + 1, rows], rsr.at[h, r + 1, rows], rs_s.at[h], rs_r.at[h, c, r], ep, ring[h]
        )

    def rs_last(h, u):
        rows = pl.ds(SUB * u, SUB)
        return remote(
            pown.at[h, NZ - 1, rows], rsr.at[h, NZ - 1, rows], rs_s.at[h], rl_r.at[h, u], ep, ring[h]
        )

    for u in range(NU):
        for h in range(2):
            with jax.named_scope("page_wait"):
                for own in range(2):
                    all_of = arr.at[u, pl.ds(0, 8 - own)]

                    @pl.when((div(ep, 8) == h) == (own == 1))
                    def _():
                        remote(all_of, all_of, a_s, a_r.at[u, h], ep, sib).wait_recv()

            paged = jnp.concatenate([arr[u, 8 * h + sl] for sl in range(8)], axis=0)
            gown[h, 0, SUB * u:SUB * (u + 1), :] = dot(perm_in[...], paged).astype(BF16)
            if u == NU - 1:
                if h == 0:
                    all_of = arr_rt.at[pl.ds(0, NEP - 1)]
                    remote(all_of, all_of, art_s, art_r, ep, sib).wait_recv()
                rts = jnp.concatenate([arr_rt[8 * h + sl] for sl in range(8)], axis=1)
                gown[h, 0, STACK:STACK + RT, :] = dot(rts, mh[...]).astype(BF16)
            ag_first(h, u).start()
    for h in range(2):
        rows_to_sib(h, 0).start()
    for s in range(2):
        for d in range(1, 4):
            for c in spread(s, d):
                c.start()

    for c in w_copies + l_copies + i_copies[5:]:
        c.wait()

    def expert(i):
        j = rem(i + 1, NZ)
        pieces = (gown.at[0, j], gown.at[1, j], gsib.at[0, i], gsib.at[1, i])
        lhs = jnp.concatenate(
            [
                jnp.concatenate([p[b * HALF:(b + 1) * HALF, :] for b in range(QB)], axis=1)
                for p in pieces
            ],
            axis=0,
        )
        diag = iota((HALF, TOK), 0) == iota((HALF, TOK), 1)
        one = jnp.ones((TOK, TOK), BF16)
        scale = []
        for p in pieces:
            tile = p[STACK:STACK + RT, 0:TOK].astype(F32)
            scale.append(
                jnp.concatenate(
                    [dot(jnp.where(diag, tile[e:e + 1, :], 0.0).astype(BF16), one) for e in range(2)],
                    axis=1,
                )
            )
        scale = jnp.concatenate(scale, axis=0)
        gate = dot(lhs, wg[...], 1, 1)
        upv = dot(lhs, wu[...], 1, 1)
        hidden = (gate / (1.0 + jnp.exp(-gate)) * upv * scale).astype(BF16)
        outs = (pown.at[0, j], pown.at[1, j], tosib.at[0, rem(i, 2)], tosib.at[1, rem(i, 2)])

        @pl.when(i >= 2)
        def _():
            for h in range(2):
                sums_to_sib(h, i - 2).wait_send()

        for b in range(0, QB, 2):
            prod = dot(hidden, wd[:, b * CW:(b + 2) * CW]).astype(BF16)
            for n, o in enumerate(outs):
                for k in range(2):
                    o[(b + k) * HALF:(b + k + 1) * HALF, :] = prod[
                        n * HALF:(n + 1) * HALF, k * CW:(k + 1) * CW
                    ]
        for h in range(2):
            sums_to_sib(h, i).start()

    def attention_ready():
        for s in range(2):
            for n in range(3):
                three = kraw.at[pl.ds(0, 3)]
                remote(three, three, t_s.at[s, n], t_r.at[s, n], ep, sib).wait_recv()

        @pl.loop(0, 8)
        def _(n):
            s = div(n, 4)
            chunk = (1 - s) * (4 * y + n) + s * (x + 4 * (n - 4))
            g = gate_ref[s, :, pl.ds(pl.multiple_of(chunk * SEG, SEG), SEG)]
            d = g[:, SEG - 1:SEG] - g
            hi = d.astype(BF16).astype(F32)
            mid = (d - hi).astype(BF16).astype(F32)
            lo = d - hi - mid
            r = iota((8, SEG), 0)
            rows = jnp.where(r == 0, hi, jnp.where(r == 1, mid, jnp.where(r == 2, lo, 0.0)))
            feats = kraw[n].astype(F32) * 0.125
            full = jnp.concatenate([feats, rows, jnp.zeros((56, SEG), F32)], axis=0)
            kt[n] = full.T.astype(BF16)

    n_first = 4 * (3 - y) + x + 1

    def unit(b):
        s = (b >= n_first).astype(jnp.int32)
        u0 = b
        late0 = (u0 > x).astype(jnp.int32)
        t0 = late0 * (u0 - x - 1)
        k0 = y + late0 * (1 + div(t0, 4))
        m0 = late0 * rem(t0, 4) + (1 - late0) * u0
        d0 = (u0 == x).astype(jnp.int32)
        u1 = s * (b - n_first)
        late1 = (u1 >= 4 * y).astype(jnp.int32)
        k1 = late1 * y + (1 - late1) * div(u1, 4)
        m1 = late1 * (x + u1 - 4 * y) + (1 - late1) * rem(u1, 4)
        d1 = (u1 == 4 * y).astype(jnp.int32)
        qs = (1 - s) * k0 + s * (4 + m1)
        kv = (1 - s) * m0 + s * (4 + k1)
        qc = (1 - s) * (4 * k0 + x) + s * (4 * y + m1)
        kc = (1 - s) * (4 * y + m0) + s * (x + 4 * k1)
        slack = (1 - ((1 - s) * d0 + s * d1)) * (2 * SEG)
        qs, kv = rem(qs, 8), rem(kv, 8)
        qc, kc = rem(qc, NEP), rem(kc, NEP)
        ref_end = gate_ref[s, :, pl.ds(pl.multiple_of(kc * SEG + SEG - 128, 128), 128)][:, 127:128]

        for at in range(0, SEG, TILE):
            lanes = slice(at, at + TILE)
            sc = dot(kt[kv], qaug[qs, :, lanes])
            keep = iota((SEG, TILE), 0) <= iota((SEG, TILE), 1) + (slack + at)
            sc = jnp.where(keep, sc, NEG)
            peak = jnp.max(sc, axis=0, keepdims=True)
            o = dot(vaug[kv], jnp.exp(sc - peak).astype(BF16))
            gq = gate_ref[s, :, pl.ds(pl.multiple_of(qc * SEG + at, TILE), TILE)]
            peak = peak + (gq - ref_end)
            old = acc[qs, 72:73, lanes]
            new = jnp.maximum(old, peak)
            acc[qs, 0:72, lanes] = acc[qs, 0:72, lanes] * jnp.exp(old - new) + o[0:72] * jnp.exp(peak - new)
            acc[qs, 72:ACC, lanes] = jnp.broadcast_to(new, (ACC - 72, TILE))

    def give(s, d):
        e = along(1 - s, d)
        mine = q_own[s] - 4 * s
        theirs = 4 * s + rem(mine + d, 4)
        return remote(acc.at[theirs], orecv.at[s, d - 1], o_s.at[s], o_r.at[s], e, tp)

    UNITS = 17
    PER = 5

    @pl.loop(0, NZ)
    def _(i):
        @pl.when(i < NZ - 1)
        def _():
            for u in range(2):
                for h in range(2):
                    with jax.named_scope("rows_wait"):
                        ag(h, u, i).wait_recv()

                    @pl.when(i < NZ - 2)
                    def _():
                        ag(h, u, i + 1).start()

            for h in range(2):
                rows_to_sib(h, i + 1).start()

        rows_from_sib(i).wait_recv()
        with jax.named_scope("expert"):
            expert(i)

        @pl.loop(0, PER)
        def _(n):
            b = PER * (i - 2) + n - 1

            @pl.when((b >= 0) & (b < UNITS))
            def _():
                with jax.named_scope("unit"):
                    unit(b)

            @pl.when((i >= 1) & (n == 0))
            def _():
                r = i - 1
                with jax.named_scope("sib_wait"):
                    sums_from_sib(i).wait_recv()
                for u in range(2):
                    for h in range(2):

                        @pl.when(r >= 1)
                        def _():
                            with jax.named_scope("sums_wait"):
                                rs(h, u, r - 1).wait_recv()

                        rows = slice(BIG * u, BIG * (u + 1))
                        pown[h, i, rows, :] = (
                            pown[h, i, rows, :].astype(F32)
                            + sibr[h, i, rows, :].astype(F32)
                            + rsr[h, r, rows, :].astype(F32)
                        ).astype(BF16)

                        @pl.when(r < NZ - 2)
                        def _():
                            rs(h, u, r).start()

                        @pl.when(r == NZ - 2)
                        def _():
                            for k in range(2):
                                rs_last(h, 2 * u + k).start()

            @pl.when((i == 2) & (n == 0))
            def _():
                with jax.named_scope("attention_ready"):
                    attention_ready()

        @pl.when(i == 5)
        def _():
            for s in range(2):
                for d in range(1, 4):
                    give(s, d).start()

    def back(e, u):
        return remote(retp.at[u, e], ret.at[u, ep], b_s, b_r.at[u], e, tp)

    sums_from_sib(0).wait_recv()
    for u in range(NU):
        for h in range(2):
            with jax.named_scope("last_wait"):
                rs_last(h, u).wait_recv()
            rows = slice(SUB * u, SUB * (u + 1))
            total = (
                pown[h, 0, rows, :].astype(F32)
                + sibr[h, 0, rows, :].astype(F32)
                + rsr[h, NZ - 1, rows, :].astype(F32)
            ).astype(BF16)
            paged = dot(perm_out[...], total).astype(BF16)
            for sl in range(8):
                src = 8 * h + sl
                retp[u, src] = paged[sl * SPAGE:(sl + 1) * SPAGE, :]

                @pl.when(src != ep)
                def _():
                    back(src, u).start()

    for u in range(NU):
        ret[u, ep] = retp[u, ep]

    for s in range(2):
        mine = q_own[s] - 4 * s
        three = orecv.at[s]
        remote(three, three, o_s.at[s], o_r.at[s], ep, sib).wait_recv()
        parts = [acc.at[q_own[s]]] + [orecv.at[s, n] for n in range(3)]
        peaks = [p[72:73, :] for p in parts]
        top = jnp.maximum(jnp.maximum(peaks[0], peaks[1]), jnp.maximum(peaks[2], peaks[3]))
        mix = sum(p[0:72, :] * jnp.exp(m - top) for p, m in zip(parts, peaks))
        att_ref[s] = (mix[0:HEAD] / mix[HEAD:HEAD + 1]).astype(BF16)

    def sends_done():
        sent = pages.at[pl.ds(0, NU), pl.ds(0, NEP - 1)]
        remote(sent, sent, a_s, a_r.at[0, 0], ep, sib).wait_send()
        sent = pages_rt.at[pl.ds(0, NEP - 1)]
        remote(sent, sent, art_s, art_r, ep, sib).wait_send()
        for s in range(2):
            three = kraw.at[pl.ds(0, 3)]
            for n in range(3):
                remote(three, three, t_s.at[s, n], t_r.at[s, n], ep, sib).wait_send()
            three = orecv.at[s]
            remote(three, three, o_s.at[s], o_r.at[s], ep, sib).wait_send()
        for h in range(2):
            sent = gown.at[h, pl.ds(0, NZ - 1)]
            remote(sent, sent, ag_s.at[h], ag_r.at[h, 0, 0], ep, sib).wait_send()
            sent = pown.at[h, pl.ds(0, NZ - 1)]
            remote(sent, sent, rs_s.at[h], rs_r.at[h, 0, 0], ep, sib).wait_send()
            sent = gown.at[h]
            remote(sent, sent, dr_s.at[h], dr_r.at[0], ep, sib).wait_send()
            for i in range(NZ - 2, NZ):
                sums_to_sib(h, i).wait_send()

    with jax.named_scope("sent"):
        sends_done()

    for u in range(NU):
        with jax.named_scope("return_wait"):
            all_of = ret.at[u, pl.ds(0, NEP - 1)]
            remote(all_of, all_of, b_s, b_r.at[u], ep, sib).wait_recv()

        with jax.named_scope("unpack"):
            back_rows = jnp.concatenate([ret[u, g] for g in range(NEP)], axis=0)
            placed = dot(pt[...], back_rows).astype(BF16)
            for b in range(UB):
                at = (b + u * UB) * CW
                out_ref[:, at:at + CW] = placed[b * TOK:(b + 1) * TOK, :]

    sent = retp.at[pl.ds(0, NU), pl.ds(0, NEP - 1)]
    remote(sent, sent, b_s, b_r.at[0], ep, sib).wait_send()


def local(
    queries, key_vectors, value_vectors, cumulative_gate, expert_input, norm_gain,
    group_choice, group_weight, expert_logits, gate_weight, up_weight, down_weight,
):
    vmem = pl.BlockSpec(memory_space=pltpu.VMEM)
    hbm = pl.BlockSpec(memory_space=pltpu.HBM)
    dma = pltpu.SemaphoreType.DMA
    v = pltpu.VMEM
    scratch = [
        v((2, 1, NEP * SEG), F32), v((TOK, DIM), BF16), v((1, DIM), F32), v((2, TOK), F32),
        v((1, TOK), F32), v((1, TOK), jnp.int32),
        v((256, DIM), BF16), v((256, DIM), BF16), v((256, DIM), BF16),
        v((NU, NEP, SPAGE, CW), BF16), v((NU, NEP, SPAGE, CW), BF16),
        v((NEP, RT, TOK), BF16), v((NEP, RT, TOK), BF16),
        v((NU, NEP, SPAGE, CW), BF16), v((NU, NEP, SPAGE, CW), BF16),
        v((SUB, SUB), BF16), v((SUB, SUB), BF16),
        v((8 * TOK, TOK), BF16), v((UB * TOK, NEP * SPAGE), BF16),
        v((2, NZ, STACK + RT, CW), BF16), v((2, NZ, STACK + RT, CW), BF16),
        v((2, NZ, STACK, CW), BF16), v((2, 2, STACK, CW), BF16), v((2, NZ, STACK, CW), BF16),
        v((2, NZ, STACK, CW), BF16),
        v((8, HEAD, SEG), BF16), v((8, ACC, SEG), BF16), v((8, 2 * HEAD, SEG), BF16),
        v((8, SEG, 2 * HEAD), BF16), v((8, ACC, SEG), F32), v((2, 3, ACC, SEG), F32),
        dma((6,)), dma((3,)), dma((6,)), dma(()), dma((NU, 2)), dma(()), dma(()), dma(()), dma((NU,)),
        dma((2,)), dma((2, 2, NZ - 1)), dma((2,)), dma((NZ,)), dma((2, 2)), dma((NZ,)),
        dma((2,)), dma((2, 2, NZ - 2)), dma((2, NU)), dma((2, 3)), dma((2, 3)), dma((2,)), dma((2,)),
    ]
    return pl.pallas_call(
        body,
        out_shape=(
            jax.ShapeDtypeStruct(queries.shape, BF16),
            jax.ShapeDtypeStruct(expert_input.shape, BF16),
        ),
        in_specs=[hbm] * 12,
        out_specs=(vmem, vmem),
        scratch_shapes=scratch,
        compiler_params=pltpu.CompilerParams(
            collective_id=0, has_side_effects=True, vmem_limit_bytes=55000000
        ),
    )(
        *(
            pltpu.with_memory_space_constraint(a, pltpu.HBM)
            for a in (
                queries, key_vectors, value_vectors, cumulative_gate, expert_input, norm_gain[None],
                expert_logits.T, group_weight[None], group_choice[None],
                gate_weight.reshape(256, DIM), up_weight.reshape(256, DIM),
                down_weight.reshape(256, DIM),
            )
        )
    )


def solution(mesh):
    return jax.shard_map(
        local,
        mesh=mesh,
        in_specs=(
            P(None, "tp", "ep"),
            P(None, "tp", "ep"),
            P(None, "tp", "ep"),
            P(None, "tp", None),
            P(("ep", "tp"), None),
            P(),
            P(("ep", "tp")),
            P(("ep", "tp")),
            P(("ep", "tp"), None),
            P("ep", "tp", None),
            P("ep", "tp", None),
            P("ep", "tp", None),
        ),
        out_specs=(P(None, "tp", "ep"), P(("ep", "tp"), None)),
        check_vma=False,
    )
```
